32 devices in a mesh: gr: 2 (over x), fs: 4 (over z), tp: 4 (over y, core).
Axes of the slice: x: 2, y: 2, z: 4, core: 2. Of those that a mesh axis runs over, the one named last changes fastest.
Arguments:
- tokens: bfloat16 [4096, 2048], P(('gr', 'fs')), may hold values from -6 to 6
- routes: int32 [4096, 2], P(('gr', 'fs')), may hold values from 0 to 3, all different within a row; in each aligned block of 512 rows (0 to 511, 512 to 1023, ...) at most 384 rows name the same one
- route_weight: float32 [4096, 2], P(('gr', 'fs')), may hold values from 0.2 to 1
- gain: float32 [2048], P(('gr', 'fs')), may hold values from 0.1 to 1.9
- w_gate: bfloat16 [4, 2048, 4096], P(None, ('gr', 'fs'), 'tp'), may hold values from -0.125 to 0.125
- w_up: bfloat16 [4, 2048, 4096], P(None, ('gr', 'fs'), 'tp'), may hold values from -0.125 to 0.125
- w_down: bfloat16 [4, 2048, 4096], P(None, ('gr', 'fs'), 'tp'), may hold values from -0.09375 to 0.09375
Outputs:
- gate_out: bfloat16 [4, 2048, 4096], P('fs', None, 'tp')
- up_out: bfloat16 [4, 2048, 4096], P('fs', None, 'tp')
- down_out: bfloat16 [4, 2048, 4096], P('fs', None, 'tp')
- mixed: bfloat16 [4096, 2048], P(('gr', 'fs'), 'tp')
The draws below stay inside these ranges and needn't reach their ends.
Inputs may be any that keep to these rules, and one draw needn't show every extreme that they name: `routes`: each row names two different experts. Among the 512 rows of one device no expert is named more than 384 times, and in every draw some device names some expert exactly 384 times.
All inputs are finite; a program needn't handle non-finite values.
Results may differ from the reference program's by a relative error of at most 0.015.
Values may be sent and summed in bfloat16 or wider, within the bound.
No kernel may reach another device: no remote copies, remote signals or barrier semaphores. Data moves between devices by JAX's collectives and lax.ppermute only.
A program may use at most 128 MiB of HBM per device.

```python
import math
import jax
import jax.numpy as jnp
import numpy as np
from jax import lax

D = 2048
FF = 4096
EXPERTS = 4
TOK_DEV = 512
CAP = 384
TOKENS = 4096
N_GR = 2
N_FS = 4
N_TP = 4


def level_of(rng, extent, cuts, low, largest):
    def one(position, shards_of):
        heights = jax.random.uniform(jax.random.fold_in(jax.random.fold_in(rng, 6), position), (shards_of,), jnp.float32, low / len(cuts), largest / len(cuts))
        return jnp.repeat(jnp.exp(heights), extent[position] // shards_of).reshape((-1,) + (1,) * (len(extent) - position - 1))

    factor_of = one(*cuts[0])
    for cut in cuts[1:]:
        factor_of = factor_of * one(*cut)
    return factor_of


def deal_out(own_key, own, number, rows, amount, top, bound, skew):
    order = jax.random.permutation(own_key, amount)
    heavy_load, ordinary = portions_of(amount, rows * top, bound, skew, True), portions_of(amount, rows * top, bound, skew, False)
    places = jnp.arange(amount)

    def named(tallies, rotation):
        used = int((tallies > 0).sum())
        fixed = max(1, used // 4)
        passed = fixed + (places - fixed + rotation * (used - fixed)) % max(1, amount - fixed)
        return jnp.zeros((amount,), jnp.int32).at[order[jnp.where(places < fixed, places, passed)]].set(jnp.asarray(tallies, jnp.int32))

    tallies = jnp.where(number % 4 == 0, named(heavy_load, number // 4), named(ordinary, number - number // 4 - 1))
    mixed = jax.random.permutation(jax.random.fold_in(own, 3), amount)
    donor, sink = mixed[0:amount // 2 * 2:2], mixed[1:amount // 2 * 2:2]
    margin = jnp.minimum(tallies[donor] - 1, bound - tallies[sink]) // 2
    margin = jnp.where((donor == order[0]) | (sink == order[0]) | (tallies[sink] == 0), 0, jnp.maximum(margin, 0))
    passed = jax.random.randint(jax.random.fold_in(own, 4), (amount // 2,), 0, 1 << 20) % (margin + 1)
    tallies = tallies.at[donor].add(-passed).at[sink].add(passed)
    members = jnp.searchsorted(jnp.cumsum(tallies), jnp.arange(rows * top), side="right").astype(jnp.int32)
    table = members.reshape(top, rows).T
    table = table[jax.random.permutation(jax.random.fold_in(own, 1), rows)]
    rotation = jax.random.randint(jax.random.fold_in(own, 2), (rows, 1), 0, top)
    return jnp.take_along_axis(table, (jnp.arange(top)[None, :] + rotation) % top, axis=1)


def portions_of(number_of, total, most, slope, full):
    portions = [(1 << 20) // math.isqrt(standing ** slope) + 1 for standing in range(1, number_of + 1)]
    largest = most if full else min(most, max(-(-total // number_of), total * portions[0] // sum(portions)))
    least = 1 if total - largest >= number_of - 1 else 0
    counts, spare = [largest] + [least] * (number_of - 1), total - largest - least * (number_of - 1)
    while spare > 0:
        candidates = [i for i in range(1, number_of) if counts[i] < largest] or [i for i in range(1, number_of) if counts[i] < most]
        pool, budget = sum([portions[i] for i in candidates]), spare
        for i in candidates:
            extra = min(most - counts[i], max(1, budget * portions[i] // pool), spare)
            counts[i] = counts[i] + extra
            spare = spare - extra
    return np.array(counts)


def gaussian(stream_key, shape, scale, most, shards=(), kind=jnp.bfloat16):
    level = level_of(stream_key, shape, shards, -0.22, 0.18) if shards else 1.0
    drawn = jax.random.normal(stream_key, shape, jnp.float32) * scale * level
    return jnp.minimum(jnp.maximum(drawn, -most), most).astype(kind)


def setup_inputs(seed: int = 0) -> dict:
    keys = jax.random.split(jax.random.key(seed), 8)
    tokens = gaussian(keys[0], (TOKENS, D), 1.0, 6.0, ((0, 8),))
    routes_keys = jax.random.split(jax.random.fold_in(keys[1], 1), TOKENS // TOK_DEV)
    routes_turns = jax.random.permutation(jax.random.fold_in(keys[1], 3), TOKENS // TOK_DEV)
    routes = jax.vmap(lambda own, number: deal_out(jax.random.fold_in(keys[1], 2), own, number, TOK_DEV, EXPERTS, 2, CAP, 2))(routes_keys, routes_turns).reshape((TOKENS, 2))
    route_weight = jnp.clip(jnp.exp(math.log(1.0) - 1.609438 * jax.random.uniform(keys[2], (TOKENS, 2), jnp.float32) ** level_of(keys[2], (TOKENS, 2), ((0, 8),), -0.2, 0.2)), 0.2, 1.0)
    gain = jnp.clip(1.0 + 0.18 * jax.random.normal(keys[3], (D,), jnp.float32), 0.1, 1.9)
    w_gate = gaussian(keys[4], (EXPERTS, D, FF), D ** -0.5, 0.125, ((1, 8), (2, 4)))
    w_up = gaussian(keys[5], (EXPERTS, D, FF), D ** -0.5, 0.125, ((1, 8), (2, 4)))
    w_down = gaussian(keys[6], (EXPERTS, D, FF), FF ** -0.5, 0.09375, ((1, 8), (2, 4)))
    return dict(tokens=tokens, routes=routes, route_weight=route_weight, gain=gain, w_gate=w_gate, w_up=w_up, w_down=w_down)


EPSILON = 1e-05

def expert_rows(pieces):
    rows, gate_w, up_w, down_w = pieces
    gate = jnp.dot(rows, gate_w, preferred_element_type=jnp.float32)
    upper = jnp.dot(rows, up_w, preferred_element_type=jnp.float32)
    hidden = (jax.nn.silu(gate) * upper).astype(jnp.bfloat16)
    count = rows.shape[0]
    blocked = hidden.reshape(count, N_TP, FF // N_TP).astype(jnp.float32)
    down_blocks = down_w.reshape(D, N_TP, FF // N_TP).astype(jnp.float32)
    partial_value = jnp.einsum('rjf,djf->jrd', blocked, down_blocks)
    rounded = lax.optimization_barrier(partial_value.astype(jnp.bfloat16))
    return lax.optimization_barrier(jnp.sum(rounded.astype(jnp.float32), axis=0)).astype(jnp.bfloat16)

def reference(tokens, routes, route_weight, gain, w_gate, w_up, w_down):
    scaling = gain[None, :, None]
    gate_out = (w_gate.astype(jnp.float32) * scaling).astype(jnp.bfloat16)
    up_out = (w_up.astype(jnp.float32) * scaling).astype(jnp.bfloat16)
    down_out = w_down
    float_rows = tokens.astype(jnp.float32)
    normed = (float_rows * lax.rsqrt(lax.optimization_barrier(jnp.mean(float_rows * float_rows, axis=-1, keepdims=True)) + EPSILON)).astype(jnp.bfloat16)
    groups = N_GR * N_FS
    flat_ids = routes.reshape(groups, TOK_DEV * 2)
    onehot = (flat_ids[:, :, None] == jnp.arange(EXPERTS, dtype=jnp.int32)[None, None, :]).astype(jnp.int32)
    slot_rank = lax.optimization_barrier(jnp.sum((jnp.cumsum(onehot, axis=1) - onehot) * onehot, axis=-1))
    group_ids = jnp.arange(groups, dtype=jnp.int32)[:, None]
    destination = (flat_ids * (groups * CAP) + group_ids * CAP + slot_rank).reshape(-1).astype(jnp.int32)
    token_ids = (jnp.arange(TOKENS * 2, dtype=jnp.int32) // 2).astype(jnp.int32)
    source = jnp.zeros((EXPERTS * groups * CAP,), jnp.int32).at[destination].set(token_ids)
    gathered = normed[source].reshape(EXPERTS, groups * CAP, D)
    outputs = lax.map(expert_rows, (gathered, gate_out, up_out, down_out))
    flat_out = outputs.reshape(EXPERTS * groups * CAP, D)
    picked = flat_out[destination].reshape(TOKENS, 2, D).astype(jnp.float32)
    mixed = lax.optimization_barrier(jnp.sum(route_weight[:, :, None] * picked, axis=1)).astype(jnp.bfloat16)
    return (gate_out, up_out, down_out, mixed)
```

```python
import jax
import jax.numpy as jnp
from jax import lax
from jax.sharding import PartitionSpec as P

EPSILON = 1e-05


def make_body(n_gr, n_fs, n_tp):
    def shift_fs(v, s):
        return lax.ppermute(v, "fs", [(i, (i + s) % n_fs) for i in range(n_fs)])

    def shift_gr(v, s):
        return lax.ppermute(v, "gr", [(i, (i + s) % n_gr) for i in range(n_gr)])

    def swap_tp(v, bit):
        return lax.ppermute(v, "tp", [(i, i ^ bit) for i in range(n_tp)])

    def body(tokens, routes, route_weight, gain, w_gate, w_up, w_down):
        fs_id, gr_id, tp_id = (lax.axis_index(a) for a in ("fs", "gr", "tp"))
        own = w_gate.shape[0] // n_fs
        rows = w_gate.shape[1]
        tok_rows, width = tokens.shape
        part = width // n_tp
        experts = own * n_fs
        capacity = 3 * tok_rows // experts
        to_id = [(fs_id + s) % n_fs for s in range(n_fs)]
        from_id = [(fs_id - s) % n_fs for s in range(n_fs)]

        def block_for(w, s):
            return lax.dynamic_slice_in_dim(w, to_id[s] * own, own, 0)

        def reshard(pieces):
            over_fs = [p if s == 0 else shift_fs(p, s) for s, p in enumerate(pieces)]
            out = jnp.zeros((own, rows * n_fs * n_gr, pieces[0].shape[-1]), jnp.bfloat16)
            for s in range(n_fs):
                for r in range(n_gr):
                    got = over_fs[s] if r == 0 else shift_gr(over_fs[s], r)
                    at = (((gr_id - r) % n_gr) * n_fs + from_id[s]) * rows
                    out = lax.dynamic_update_slice(out, got, (0, at, 0))
            return out

        scaling = gain[None, :, None]

        def scaled(w, s):
            return (block_for(w, s).astype(jnp.float32) * scaling).astype(jnp.bfloat16)

        gate_out = reshard([scaled(w_gate, s) for s in range(n_fs)])
        up_out = reshard([scaled(w_up, s) for s in range(n_fs)])
        down_out = reshard([block_for(w_down, s) for s in range(n_fs)])

        float_rows = tokens.astype(jnp.float32)
        norm = lax.rsqrt(jnp.mean(float_rows * float_rows, axis=-1, keepdims=True) + EPSILON)
        my_cols = lax.dynamic_slice_in_dim(tokens, tp_id * part, part, 1)
        normed = (my_cols.astype(jnp.float32) * norm).astype(jnp.bfloat16)
        flat_ids = routes.reshape(-1)
        onehot = (flat_ids[:, None] == jnp.arange(experts, dtype=jnp.int32)[None, :]).astype(jnp.int32)
        slot_rank = jnp.sum((jnp.cumsum(onehot, axis=0) - onehot) * onehot, axis=-1)
        destination = (flat_ids * capacity + slot_rank).reshape(tok_rows, 2)
        block = own * capacity
        slots = [to_id[s] * block + jnp.arange(block, dtype=jnp.int32) for s in range(n_fs)]
        arrived = []
        for s in range(n_fs):
            hits = slots[s][:, None, None] == destination[None, :, :]
            dispatch = jnp.any(hits, axis=-1).astype(jnp.bfloat16)
            out = jnp.dot(dispatch, normed, preferred_element_type=jnp.float32).astype(jnp.bfloat16)
            arrived.append(out if s == 0 else shift_fs(out, s))
        cols = {0: jnp.concatenate(arrived, axis=0)}
        bit = n_tp // 2
        while bit:
            for k in list(cols):
                cols[k | bit] = swap_tp(cols[k], bit)
            bit //= 2
        rows_in = jnp.zeros((n_fs * block, width), jnp.bfloat16)
        for k, v in cols.items():
            rows_in = lax.dynamic_update_slice(rows_in, v, (0, (tp_id ^ k) * part))

        rows_in = rows_in.reshape(n_fs, own, capacity, width)
        gate = jnp.einsum("sjnd,jdf->sjnf", rows_in, gate_out, preferred_element_type=jnp.float32)
        upper = jnp.einsum("sjnd,jdf->sjnf", rows_in, up_out, preferred_element_type=jnp.float32)
        hidden = (jax.nn.silu(gate) * upper).astype(jnp.bfloat16)

        mixed = jnp.zeros((tok_rows, part), jnp.float32)
        down_cols = [
            lax.dynamic_slice_in_dim(down_out, (tp_id ^ k) * part, part, 1) for k in range(n_tp)
        ]
        for s in range(n_fs):
            pieces = {}
            for k in reversed(range(n_tp)):
                pieces[k] = jnp.einsum(
                    "jnf,jdf->jnd", hidden[s], down_cols[k], preferred_element_type=jnp.float32
                )
            bit = 1
            while bit < n_tp:
                for k in sorted(pieces, reverse=True):
                    if k & bit:
                        got = swap_tp(pieces.pop(k).astype(jnp.bfloat16), bit)
                        pieces[k ^ bit] = pieces[k ^ bit] + got.astype(jnp.float32)
                bit *= 2
            back = pieces[0].astype(jnp.bfloat16)
            if s:
                back = shift_fs(back, -s)
            first = jnp.where(slots[s][None, :] == destination[:, 0:1], route_weight[:, 0:1], 0.0)
            second = jnp.where(slots[s][None, :] == destination[:, 1:2], route_weight[:, 1:2], 0.0)
            pick = first + second
            high = pick.astype(jnp.bfloat16)
            low = (pick - high.astype(jnp.float32)).astype(jnp.bfloat16)
            back = back.reshape(block, part)
            mixed = mixed + jnp.dot(high, back, preferred_element_type=jnp.float32)
            mixed = mixed + jnp.dot(low, back, preferred_element_type=jnp.float32)
        return (gate_out, up_out, down_out, mixed.astype(jnp.bfloat16))

    return body


def solution(mesh):
    in_specs = (
        P(("gr", "fs"), None),
        P(("gr", "fs"), None),
        P(("gr", "fs"), None),
        P(("gr", "fs")),
        P(None, ("gr", "fs"), "tp"),
        P(None, ("gr", "fs"), "tp"),
        P(None, ("gr", "fs"), "tp"),
    )
    out_specs = (
        P("fs", None, "tp"),
        P("fs", None, "tp"),
        P("fs", None, "tp"),
        P(("gr", "fs"), "tp"),
    )
    body = make_body(*(mesh.shape[a] for a in ("gr", "fs", "tp")))
    return jax.shard_map(body, mesh=mesh, in_specs=in_specs, out_specs=out_specs, check_vma=False)
```
